32 devices in a mesh: grp: 2 (over y), fs: 4 (over z), tp: 4 (over x, core).
Axes of the slice: x: 2, y: 2, z: 4, core: 2. Of those that a mesh axis runs over, the one named last changes fastest.
Arguments:
- tokens: bfloat16 [4096, 2048], P(('grp', 'fs', 'tp')), parts along dimension 0, may hold values from -6 to 6
- up_master: float32 [2048, 4096], P('fs', 'tp'), may hold values from -0.125 to 0.125
- down_master: float32 [4096, 2048], P('fs', 'tp'), may hold values from -0.09375 to 0.09375
- norm_gain: float32 [2048], P('fs'), may hold values from 0.1 to 1.9
Outputs:
- up_weights: bfloat16 [4096, 4096], P('grp', 'tp'), parts along dimension 0
- down_weights: bfloat16 [8192, 2048], P(('grp', 'tp')), parts along dimension 0
- mlp_output: bfloat16 [4096, 2048], P(('grp', 'fs', 'tp')), parts along dimension 0
The draws below stay inside these ranges and needn't reach their ends.
There are 2 independent parts, one for each index of `grp`. The reference program is written for one: setup_inputs(seed, part) draws one part's arguments, and reference() takes and returns one part's arrays. A program takes and returns all parts, laid end to end along the dimension named above; an argument that names none is the same for every part. Nothing has to cross between parts.
All inputs are finite; a program needn't handle non-finite values.
Results may differ from the reference program's by a relative error of at most 0.014.
Values may be sent and summed in bfloat16 or wider, within the bound.
A program may use at most 64 MiB of HBM per device.

```python
import jax
import jax.numpy as jnp
from jax import lax

D = 2048
FF = 4096
TOKENS = 2048
N_TP = 4


def steps_of(stream_key, dims, split, smallest, top_value):
    level = 1.0
    for dim, blocks in split:
        steps = jax.random.uniform(jax.random.fold_in(jax.random.fold_in(stream_key, 6), dim), (blocks,), jnp.float32, smallest / len(split), top_value / len(split))
        level = level * jnp.repeat(jnp.exp(steps), dims[dim] // blocks).reshape((-1,) + (1,) * (len(dims) - 1 - dim))
    return level


def centred(stream_key, shape, deviation, bound, cuts=(), dtype=jnp.bfloat16):
    entries = deviation * jax.random.normal(stream_key, shape, jnp.float32)
    if cuts:
        entries = entries * steps_of(stream_key, shape, cuts, -0.22, 0.18)
    return jnp.clip(entries, -bound, bound).astype(dtype)


def setup_inputs(seed: int = 0, part: int = 0) -> dict:
    keys = jax.random.split(jax.random.key(seed), 5)
    part_splits = jax.random.split(jax.random.fold_in(keys[4], part), 5)
    tokens = centred(part_splits[0], (TOKENS, D), 1.0, 6.0, ((0, 16),))
    up_master = centred(keys[1], (D, FF), D ** -0.5, 0.125, ((0, 4), (1, 4)), jnp.float32)
    down_master = centred(keys[2], (FF, D), FF ** -0.5, 0.09375, ((0, 4), (1, 4)), jnp.float32)
    norm_gain = jnp.clip(1.0 + 0.18 * jax.random.normal(keys[3], (D,), jnp.float32), 0.1, 1.9)
    return dict(tokens=tokens, up_master=up_master, down_master=down_master, norm_gain=norm_gain)


def reference(tokens, up_master, down_master, norm_gain):
    up_weights = (norm_gain[:, None] * up_master).astype(jnp.bfloat16)
    down_weights = down_master.astype(jnp.bfloat16)
    float_tokens = tokens.astype(jnp.float32)
    scale = lax.rsqrt(lax.optimization_barrier(jnp.mean(float_tokens * float_tokens, axis=-1, keepdims=True)) + 1e-06)
    normed = (float_tokens * scale).astype(jnp.bfloat16)
    preact = jnp.dot(normed, up_weights, preferred_element_type=jnp.float32)
    rectified = jax.nn.relu(preact)
    hidden = (rectified * rectified).astype(jnp.bfloat16)
    row_total = hidden.shape[0]
    block_width = FF // N_TP
    hidden_blocks = hidden.reshape(row_total, N_TP, block_width).transpose(1, 0, 2)
    down_blocks = down_weights.reshape(N_TP, block_width, D)

    def accumulate(running, operands):
        hidden_block, down_block = operands
        partial_value = jnp.dot(hidden_block, down_block, preferred_element_type=jnp.float32).astype(jnp.bfloat16)
        partial_value = lax.optimization_barrier(partial_value)
        return (running + partial_value.astype(jnp.float32), None)
    start_sum = jnp.zeros((row_total, D), jnp.float32)
    summed, _ = lax.scan(accumulate, start_sum, (hidden_blocks, down_blocks))
    return (up_weights, down_weights, summed.astype(jnp.bfloat16))
```

```python
import functools

import jax
import jax.numpy as jnp
from jax import lax
from jax.experimental import pallas as pl
from jax.experimental.pallas import tpu as pltpu
from jax.sharding import PartitionSpec as P

MESH = pl.DeviceIdType.MESH


def pieces(size, unit, most):
    count = most
    while count > 1 and size % (count * unit):
        count -= 1
    return count


def counts(G, F, T, r, rd, cd):
    C = pieces(r // G, 16, 2)
    J = pieces(cd, 128, 2)
    if F > 8:
        C, J = 1, 1
    return C, J, F // T


def kernel(G, F, T, C, J, m, tok_in, up_in, down_in, up_out, down_out, mlp_out,
           nrm, upw, dnw, hidden, pout, part, acc,
           send, rup, yup, rdn, ydn, rtok, rpart, loc):
    g, f, k = lax.axis_index("grp"), lax.axis_index("fs"), lax.axis_index("tp")
    r, cu = up_in.shape
    rd, cd = down_in.shape
    R, D = tok_in.shape
    h, hd, w = r // G, rd // G, cd // J
    hc = h // C
    home = f // m
    mine = k == home
    slot = f % m

    def column_owner(dev, p):
        if T % 2:
            return (dev + p) % T
        return ((dev // 2 + p // 2) % (T // 2)) * 2 + (dev + p) % 2

    def position_of(owner, dev):
        if T % 2:
            return (owner + T - dev) % T
        return ((owner // 2 + T // 2 - dev // 2) % (T // 2)) * 2 + (owner + dev) % 2

    local = []

    def keep(cond, src, dst):
        copy = pltpu.make_async_copy(src, dst, loc.at[len(local)])
        local.append(cond)
        if cond is None:
            copy.start()
        else:
            pl.when(cond)(copy.start)
        return copy

    own_up = keep(None, up_in, upw.at[pl.ds(pl.multiple_of(f * r, r), r)])
    own_tok = keep(None, tok_in, nrm.at[pl.ds(pl.multiple_of(k * R, R), R)])
    own_down = keep(mine, down_in, dnw.at[pl.ds(pl.multiple_of(slot * rd, rd), rd), pl.ds(pl.multiple_of(k * cd, cd), cd)])

    barrier = pltpu.get_barrier_semaphore()

    def greet(**where):
        pl.semaphore_signal(barrier, inc=1, device_id=where, device_id_type=MESH)

    for e in range(1, G):
        greet(grp=(g + e) % G)
    for d in range(1, T):
        greet(tp=(k + d) % T)

    @pl.when(f > 0)
    def _():
        greet(fs=f - 1)

    @pl.when(f < F - 1)
    def _():
        greet(fs=f + 1)

    pl.semaphore_wait(barrier, G - 1 + T - 1 + (f > 0).astype(jnp.int32) + (f < F - 1).astype(jnp.int32))

    sent = []

    def put(cond, src, dst, sem, where):
        copy = pltpu.make_async_remote_copy(
            src_ref=src, dst_ref=dst, send_sem=send.at[len(sent)], recv_sem=sem,
            device_id=where, device_id_type=MESH)
        sent.append((cond, copy))
        if cond is None:
            copy.start()
        else:
            pl.when(cond)(copy.start)

    def arrived(ref, sem, where):
        pltpu.make_async_remote_copy(
            src_ref=ref, dst_ref=ref, send_sem=send.at[0], recv_sem=sem,
            device_id=where, device_id_type=MESH).wait_recv()

    def up_piece(s, part_of, c):
        return upw.at[pl.ds(pl.multiple_of(s * r + part_of * h + c * hc, hc), hc)]

    def down_piece(si, p, j, part_of):
        t = column_owner(k, p)
        return dnw.at[pl.ds(pl.multiple_of(si * rd + part_of * hd, hd), hd),
                      pl.ds(pl.multiple_of(t * cd + j * w, w), w)]

    for c in range(C):
        src = up_in.at[pl.ds(pl.multiple_of(g * h + c * hc, hc), hc)]
        put(f < F - 1, src, up_piece(f, g, c), rup.at[0, 0, c], {"fs": f + 1})
        put(f > 0, src, up_piece(f, g, c), rup.at[1, 0, c], {"fs": f - 1})

    place = position_of(k, home)
    for j in range(J):
        put(jnp.logical_not(mine),
            down_in.at[pl.ds(pl.multiple_of(g * hd, hd), hd), pl.ds(j * w, w)],
            dnw.at[pl.ds(pl.multiple_of(slot * rd + g * hd, hd), hd), pl.ds(pl.multiple_of(k * cd + j * w, w), w)],
            rdn.at[slot, place, j], {"tp": home})
    for d in range(1, T):
        put(None, tok_in, nrm.at[pl.ds(pl.multiple_of(k * R, R), R)], rtok.at[d - 1], {"tp": (k + d) % T})

    own_up.wait()
    own_tok.wait()
    pl.when(mine)(own_down.wait)

    for d in range(1, F):
        for c in range(C):
            for way in range(2):
                s = f - d if way == 0 else f + d
                here = f >= d if way == 0 else f < F - d

                @pl.when(here)
                def _(s=s, way=way):
                    arrived(up_piece(s, g, c), rup.at[way, d - 1, c], {"fs": s})

                if d < F - 1:
                    more = jnp.logical_and(here, f < F - 1 if way == 0 else f > 0)
                    put(more, up_piece(s, g, c), up_piece(s, g, c), rup.at[way, d, c],
                        {"fs": f + 1 if way == 0 else f - 1})
                for e in range(1, G):
                    put(here, up_piece(s, g, c), up_piece(s, g, c), yup.at[e - 1, way, d - 1, c],
                        {"grp": (g + e) % G})

    def down_step(p, j):
        for si in range(m):
            s = k * m + si
            block = down_piece(si, p, j, g)
            away = None if p else f != s
            sem = rdn.at[si, p, j]
            if p:
                arrived(block, sem, {"fs": f})
            else:
                @pl.when(away)
                def _():
                    arrived(block, sem, {"fs": f})
            put(jnp.logical_and(f >= s, f < F - 1), block, block, sem, {"fs": f + 1})
            put(jnp.logical_and(f <= s, f > 0), block, block, sem, {"fs": f - 1})
            for e in range(1, G):
                put(away, block, block, ydn.at[e - 1, si, p, j], {"grp": (g + e) % G})

    stored = []

    def hidden_units():
        for d in range(1, F):
            for c in range(C):
                for way in range(2):
                    s = f - d if way == 0 else f + d
                    here = f >= d if way == 0 else f < F - d

                    @pl.when(here)
                    def _(s=s, way=way):
                        for e in range(1, G):
                            arrived(up_piece(s, (g + G - e) % G, c), yup.at[e - 1, way, d - 1, c], {"fs": f})

        stored.append(keep(None, upw, up_out))
        for d in range(1, T):
            arrived(nrm.at[pl.ds(pl.multiple_of((k + T - d) % T * R, R), R)], rtok.at[d - 1], {"fs": f})
        tile = min(cu, 256)

        @pl.loop(0, cu // tile)
        def _(i):
            cols = pl.ds(pl.multiple_of(i * tile, tile), tile)
            rect = jnp.maximum(jnp.dot(nrm[...], upw[:, cols], preferred_element_type=jnp.float32), 0.0)
            hidden[:, cols] = (rect * rect).astype(hidden.dtype)

    def output_step(p, j):
        for si in range(m):
            s = k * m + si

            def peers(si=si):
                for e in range(1, G):
                    arrived(down_piece(si, p, j, (g + G - e) % G), ydn.at[e - 1, si, p, j], {"fs": f})
            if p:
                peers()
            else:
                pl.when(f != s)(peers)
        cols = pl.ds(pl.multiple_of(column_owner(k, p) * cd + j * w, w), w)
        stored.append(keep(None, dnw.at[:, cols], down_out.at[:, cols]))
        pout[:, cols] = jnp.dot(hidden[...], dnw[:, cols], preferred_element_type=jnp.float32).astype(pout.dtype)
        for d in range(1, T):
            to = (k + d) % T
            put(None, pout.at[pl.ds(pl.multiple_of(to * R, R), R), cols], part.at[d - 1, :, cols],
                rpart.at[d - 1, p, j], {"tp": to})

    steps = [(p, j) for p in range(T) for j in range(J)]
    lag = min(2, len(steps))
    for n in range(len(steps) + lag):
        if n < len(steps):
            down_step(*steps[n])
        if n == lag - 1:
            hidden_units()
        if n >= lag:
            output_step(*steps[n - lag])

    for p, j in steps:
        for d in range(1, T):
            cols = pl.ds(pl.multiple_of(column_owner((k + T - d) % T, p) * cd + j * w, w), w)
            arrived(part.at[d - 1, :, cols], rpart.at[d - 1, p, j], {"fs": f})
    total = pout[pl.ds(pl.multiple_of(k * R, R), R), :].astype(jnp.float32)
    for d in range(1, T):
        total += part[d - 1].astype(jnp.float32)
    acc[...] = total.astype(acc.dtype)
    stored.append(keep(None, acc, mlp_out))
    for copy in stored:
        copy.wait()
    for cond, copy in sent:
        if cond is None:
            copy.wait_send()
        else:
            pl.when(cond)(copy.wait_send)


def solution(mesh):
    G, F, T = (mesh.shape[a] for a in ("grp", "fs", "tp"))

    def on_device(tokens, up_master, down_master, norm_gain):
        up_local = (norm_gain[:, None] * up_master).astype(jnp.bfloat16)
        down_local = down_master.astype(jnp.bfloat16)
        wide = tokens.astype(jnp.float32)
        scale = lax.rsqrt(jnp.mean(wide * wide, axis=-1, keepdims=True) + 1e-06)
        normed = (wide * scale).astype(jnp.bfloat16)
        (r, cu), (rd, cd), (R, D) = up_local.shape, down_local.shape, normed.shape
        C, J, m = counts(G, F, T, r, rd, cd)
        sends = (2 * C + J + T - 1 + 2 * (F - 1) * C * G + m * T * J * (G + 1) + T * J * (T - 1))
        bf16 = jnp.bfloat16
        dma = pltpu.SemaphoreType.DMA
        any_spec = pl.BlockSpec(memory_space=pl.ANY)
        return pl.pallas_call(
            functools.partial(kernel, G, F, T, C, J, m),
            out_shape=(
                jax.ShapeDtypeStruct((F * r, cu), bf16),
                jax.ShapeDtypeStruct((m * rd, T * cd), bf16),
                jax.ShapeDtypeStruct((R, D), bf16),
            ),
            in_specs=[any_spec] * 3,
            out_specs=(any_spec,) * 3,
            scratch_shapes=[
                pltpu.VMEM((T * R, D), bf16),
                pltpu.VMEM((F * r, cu), bf16),
                pltpu.VMEM((m * rd, T * cd), bf16),
                pltpu.VMEM((T * R, cu), bf16),
                pltpu.VMEM((T * R, D), bf16),
                pltpu.VMEM((T - 1, R, D), bf16),
                pltpu.VMEM((R, D), bf16),
                dma((sends,)),
                dma((2, F - 1, C)),
                dma((max(G - 1, 1), 2, F - 1, C)),
                dma((m, T, J)),
                dma((max(G - 1, 1), m, T, J)),
                dma((T - 1,)),
                dma((T - 1, T, J)),
                dma((5 + T * J,)),
            ],
            compiler_params=pltpu.CompilerParams(
                collective_id=0, has_side_effects=True, vmem_limit_bytes=44 * 2**20
            ),
        )(normed, up_local, down_local)

    in_specs = (P(("grp", "fs", "tp"), None), P("fs", "tp"), P("fs", "tp"), P("fs"))
    out_specs = (P("grp", "tp"), P(("grp", "tp"), None), P(("grp", "fs", "tp"), None))
    return jax.shard_map(
        on_device, mesh=mesh, in_specs=in_specs, out_specs=out_specs, check_vma=False
    )
```

```python
import functools

import jax
import jax.numpy as jnp
from jax import lax
from jax.experimental import pallas as pl
from jax.experimental.pallas import tpu as pltpu
from jax.sharding import PartitionSpec as P

MESH = pl.DeviceIdType.MESH
DETOUR = False
FINAL = True
VMEM_MIB = 36


def pieces(size, unit, most):
    count = most
    while count > 1 and size % (count * unit):
        count -= 1
    return count


def counts(G, F, T, r, rd, cd):
    C = pieces(r // G, 16, 2)
    J = pieces(cd, 128, 2)
    if F > 8:
        C, J = 1, 1
    return C, J, F // T


def kernel(G, F, T, C, J, m, detour, gain, tok_in, up_in, down_in, up_out, down_out, mlp_out,
           wide_up, wide_down, raw_tok, stage, alt,
           nrm, upw, dnw, hidden, pout, part, acc,
           send, rup, yup, rdn, ydn, rtok, rpart, ralt, yalt, loc):
    g, f, k = lax.axis_index("grp"), lax.axis_index("fs"), lax.axis_index("tp")
    r, cu = up_in.shape
    rd, cd = down_in.shape
    R, D = tok_in.shape
    h, hd, w = r // G, rd // G, cd // J
    hc = h // C
    home = f // m
    mine = k == home
    slot = f % m

    def column_owner(dev, p):
        if T % 2:
            return (dev + p) % T
        return ((dev // 2 + p // 2) % (T // 2)) * 2 + (dev + p) % 2

    def position_of(owner, dev):
        if T % 2:
            return (owner + T - dev) % T
        return ((owner // 2 + T // 2 - dev // 2) % (T // 2)) * 2 + (owner + dev) % 2

    local = []

    def keep(cond, src, dst):
        copy = pltpu.make_async_copy(src, dst, loc.at[len(local)])
        local.append(cond)
        if cond is None:
            copy.start()
        else:
            pl.when(cond)(copy.start)
        return copy

    load_up = keep(None, up_in, wide_up)
    load_down = keep(None, down_in, wide_down)
    load_tok = keep(None, tok_in, raw_tok)

    barrier = pltpu.get_barrier_semaphore()

    def greet(**where):
        pl.semaphore_signal(barrier, inc=1, device_id=where, device_id_type=MESH)

    for e in range(1, G):
        greet(grp=(g + e) % G)
    for d in range(1, T):
        greet(tp=(k + d) % T)

    @pl.when(f > 0)
    def _():
        greet(fs=f - 1)

    @pl.when(f < F - 1)
    def _():
        greet(fs=f + 1)

    def scale_up(half):
        rows = min(h, 128)
        for a in range(0, h, rows):
            at = pl.multiple_of(half * h + a, rows)
            column = jnp.broadcast_to(gain[:, pl.ds(at, rows)], (128, rows)).T if rows == 128 else None
            for b in range(0, cu, 128):
                block = wide_up[pl.ds(at, rows), pl.ds(b, 128)]
                factor = column if column is not None else gain_column(at, rows)
                upw[pl.ds(pl.multiple_of(f * r + at, rows), rows), pl.ds(b, 128)] = (factor * block).astype(upw.dtype)

    def gain_column(at, rows):
        lanes = lax.broadcasted_iota(jnp.int32, (rows, r), 1)
        row = lax.broadcasted_iota(jnp.int32, (rows, r), 0)
        picked = jnp.where(lanes == row + at, gain[...], 0.0)
        return jnp.sum(picked, axis=1, keepdims=True)

    def round_down(half):
        rows = pl.ds(pl.multiple_of(half * hd, hd), hd)
        for j in range(J):
            stage[j, rows, :] = wide_down[rows, pl.ds(j * w, w)].astype(stage.dtype)

    load_up.wait()
    scale_up(g)
    load_down.wait()
    round_down(g)
    pl.semaphore_wait(barrier, G - 1 + T - 1 + (f > 0).astype(jnp.int32) + (f < F - 1).astype(jnp.int32))

    sent = []

    def put(cond, src, dst, sem, where):
        copy = pltpu.make_async_remote_copy(
            src_ref=src, dst_ref=dst, send_sem=send.at[len(sent)], recv_sem=sem,
            device_id=where, device_id_type=MESH)
        sent.append((cond, copy))
        if cond is None:
            copy.start()
        else:
            pl.when(cond)(copy.start)

    def arrived(ref, sem, where):
        pltpu.make_async_remote_copy(
            src_ref=ref, dst_ref=ref, send_sem=send.at[0], recv_sem=sem,
            device_id=where, device_id_type=MESH).wait_recv()

    def up_piece(s, part_of, c):
        return upw.at[pl.ds(pl.multiple_of(s * r + part_of * h + c * hc, hc), hc)]

    def down_piece(si, p, j, part_of):
        t = column_owner(k, p)
        return dnw.at[t * J + j, pl.ds(pl.multiple_of(si * rd + part_of * hd, hd), hd)]

    if detour:
        via = ((k // 2 + 1) % (T // 2)) * 2 + (k + 1) % 2
        upward = 2 * via < T
        passing = jnp.logical_or(jnp.logical_and(upward, f > via), jnp.logical_and(jnp.logical_not(upward), f < via))
    for c in range(C):
        src = up_piece(f, g, c)
        put(f < F - 1, src, up_piece(f, g, c), rup.at[0, 0, c], {"fs": f + 1})
        put(f > 0, src, up_piece(f, g, c), rup.at[1, 0, c], {"fs": f - 1})
        if detour and c == 0:
            for j in range(J):
                src = stage.at[j, pl.ds(pl.multiple_of(g * hd, hd), hd)]
                dst = alt.at[j, pl.ds(pl.multiple_of(g * hd, hd), hd)]
                put(jnp.logical_and(upward, jnp.logical_and(f == via, f < F - 1)), src, dst, ralt.at[j], {"fs": f + 1})
                put(jnp.logical_and(jnp.logical_not(upward), jnp.logical_and(f == via, f > 0)), src, dst, ralt.at[j], {"fs": f - 1})

    place = position_of(k, home)
    for j in range(J):
        put(jnp.logical_not(mine), stage.at[j, pl.ds(pl.multiple_of(g * hd, hd), hd)],
            dnw.at[k * J + j, pl.ds(pl.multiple_of(slot * rd + g * hd, hd), hd)],
            rdn.at[slot, place, j], {"tp": home})

    for e in range(1, G):
        scale_up((g + e) % G)
        round_down((g + e) % G)
    load_tok.wait()
    wide = raw_tok[...].astype(jnp.float32)
    mean = jnp.mean(wide * wide, axis=-1, keepdims=True)
    nrm[pl.ds(pl.multiple_of(k * R, R), R), :] = (wide * lax.rsqrt(mean + 1e-06)).astype(nrm.dtype)
    held = [keep(mine, stage.at[j], dnw.at[k * J + j, pl.ds(pl.multiple_of(slot * rd, rd), rd)]) for j in range(J)]
    for copy in held:
        pl.when(mine)(copy.wait)
    def tokens_of(owner):
        return nrm.at[pl.ds(pl.multiple_of(owner * R, R), R)]

    own = tokens_of(k)
    if T % 2:
        for p in range(1, T):
            put(None, own, own, rtok.at[T - p], {"tp": column_owner(k, p)})
    else:
        for p in range(2, T, 2):
            put(None, own, own, rtok.at[T - p], {"tp": column_owner(k, p)})
        put(None, own, own, rtok.at[1], {"tp": column_owner(k, 1)})

    def pass_tokens():
        if T % 2 == 0:
            for p in range(2, T, 2):
                block = tokens_of(column_owner(k, p))
                arrived(block, rtok.at[p], {"fs": f})
                put(None, block, block, rtok.at[p + 1], {"tp": column_owner(k, 1)})

    def alt_step(j):
        block = alt.at[j, pl.ds(pl.multiple_of(g * hd, hd), hd)]

        @pl.when(passing)
        def _():
            arrived(block, ralt.at[j], {"fs": f})

        put(jnp.logical_and(passing, jnp.logical_and(upward, f < F - 1)), block, block, ralt.at[j], {"fs": f + 1})
        put(jnp.logical_and(passing, jnp.logical_and(jnp.logical_not(upward), f > 0)), block, block, ralt.at[j], {"fs": f - 1})
        for e in range(1, G):
            put(passing, block, block, yalt.at[e - 1, j], {"grp": (g + e) % G})
        put(passing, block, dnw.at[k * J + j, pl.ds(pl.multiple_of(g * hd, hd), hd)], rdn.at[0, T - 1, j], {"tp": via})

    def alt_cross(j):
        for e in range(1, G):
            rows = pl.ds(pl.multiple_of((g + G - e) % G * hd, hd), hd)

            @pl.when(passing)
            def _():
                arrived(alt.at[j, rows], yalt.at[e - 1, j], {"fs": f})

            put(passing, alt.at[j, rows], dnw.at[k * J + j, rows], ydn.at[e - 1, 0, T - 1, j], {"tp": via})

    for d in range(1, F):
        for c in range(C):
            for way in range(2):
                s = f - d if way == 0 else f + d
                here = f >= d if way == 0 else f < F - d

                @pl.when(here)
                def _(s=s, way=way):
                    arrived(up_piece(s, g, c), rup.at[way, d - 1, c], {"fs": s})

                if d < F - 1:
                    more = jnp.logical_and(here, f < F - 1 if way == 0 else f > 0)
                    put(more, up_piece(s, g, c), up_piece(s, g, c), rup.at[way, d, c],
                        {"fs": f + 1 if way == 0 else f - 1})
                for e in range(1, G):
                    put(here, up_piece(s, g, c), up_piece(s, g, c), yup.at[e - 1, way, d - 1, c],
                        {"grp": (g + e) % G})

        if d == min(2, F - 1):
            pass_tokens()
        if detour:
            for j in range(J):
                if d == 1:
                    alt_step(j)
                if d == min(2, F - 1):
                    alt_cross(j)

    def down_step(p, j):
        for si in range(m):
            s = k * m + si
            block = down_piece(si, p, j, g)
            away = None if p else f != s
            sem = rdn.at[si, p, j]
            if p:
                arrived(block, sem, {"fs": f})
            else:
                @pl.when(away)
                def _():
                    arrived(block, sem, {"fs": f})
            right = jnp.logical_and(f >= s, f < F - 1)
            left = jnp.logical_and(f <= s, f > 0)
            if detour and p == T - 1:
                low = 2 * k < T
                high = jnp.logical_not(low)
                right = jnp.logical_and(right, high)
                left = jnp.logical_and(left, low)
                away = jnp.logical_and(jnp.logical_or(high, f <= s), jnp.logical_or(low, f >= s))
            put(right, block, block, sem, {"fs": f + 1})
            put(left, block, block, sem, {"fs": f - 1})
            for e in range(1, G):
                put(away, block, block, ydn.at[e - 1, si, p, j], {"grp": (g + e) % G})

    stored = []

    def hidden_units():
        for d in range(1, F):
            for c in range(C):
                for way in range(2):
                    s = f - d if way == 0 else f + d
                    here = f >= d if way == 0 else f < F - d

                    @pl.when(here)
                    def _(s=s, way=way):
                        for e in range(1, G):
                            arrived(up_piece(s, (g + G - e) % G, c), yup.at[e - 1, way, d - 1, c], {"fs": f})

        stored.append(keep(None, upw, up_out))
        for p in range(1, T):
            if T % 2 or p % 2:
                arrived(tokens_of(column_owner(k, p)), rtok.at[p], {"fs": f})
        tile = min(cu, 256)

        @pl.loop(0, cu // tile)
        def _(i):
            cols = pl.ds(pl.multiple_of(i * tile, tile), tile)
            rect = jnp.maximum(jnp.dot(nrm[...], upw[:, cols], preferred_element_type=jnp.float32), 0.0)
            hidden[:, cols] = (rect * rect).astype(hidden.dtype)

    def output_step(p, j):
        for si in range(m):
            s = k * m + si

            def peers(si=si):
                for e in range(1, G):
                    arrived(down_piece(si, p, j, (g + G - e) % G), ydn.at[e - 1, si, p, j], {"fs": f})
            if p:
                peers()
            else:
                pl.when(f != s)(peers)
        n = column_owner(k, p) * J + j
        stored.append(keep(None, dnw.at[n], down_out.at[:, pl.ds(pl.multiple_of(n * w, w), w)]))
        pout[n] = jnp.dot(hidden[...], dnw[n], preferred_element_type=jnp.float32).astype(pout.dtype)
        for d in range(1, T):
            to = (k + d) % T
            put(None, pout.at[n, pl.ds(pl.multiple_of(to * R, R), R)], part.at[d - 1, n],
                rpart.at[d - 1, p, j], {"tp": to})

    steps = [(p, j) for p in range(T) for j in range(J)]
    first = min(4, len(steps)) - 1
    done = 0
    for n in range(len(steps)):
        down_step(*steps[n])
        if n == first:
            hidden_units()
        if n >= first:
            while done < n - 1:
                output_step(*steps[done])
                done += 1
    for step in steps[done:]:
        output_step(*step)

    for p, j in steps:
        for d in range(1, T):
            n = column_owner((k + T - d) % T, p) * J + j
            arrived(part.at[d - 1, n], rpart.at[d - 1, p, j], {"fs": f})
    own_rows = pl.ds(pl.multiple_of(k * R, R), R)
    for n in range(T * J):
        total = pout[n, own_rows, :].astype(jnp.float32)
        for d in range(1, T):
            total += part[d - 1, n].astype(jnp.float32)
        acc[:, n * w:(n + 1) * w] = total.astype(acc.dtype)
    stored.append(keep(None, acc, mlp_out))
    for copy in stored:
        copy.wait()
    for cond, copy in sent:
        if cond is None:
            copy.wait_send()
        else:
            pl.when(cond)(copy.wait_send)


def place(a, b, c, x, y, z, sems):
    copies = [pltpu.make_async_copy(i, o, sems.at[n]) for n, (i, o) in enumerate(((a, x), (b, y), (c, z)))]
    for copy in copies:
        copy.start()
    for copy in copies:
        copy.wait()


def solution(mesh):
    G, F, T = (mesh.shape[a] for a in ("grp", "fs", "tp"))

    def on_device(tokens, up_master, down_master, norm_gain):
        (r, cu), (rd, cd), (R, D) = up_master.shape, down_master.shape, tokens.shape
        C, J, m = counts(G, F, T, r, rd, cd)
        w = cd // J
        detour = DETOUR and m == 1 and T % 2 == 0 and T > 2
        sends = 2 * J + J * (2 * G + 2) + (2 * C + J + T - 1 + 2 * (F - 1) * C * G + m * T * J * (G + 1) + T * J * (T - 1))
        bf16 = jnp.bfloat16
        dma = pltpu.SemaphoreType.DMA
        any_spec = pl.BlockSpec(memory_space=pl.ANY)
        held = pl.pallas_call(
            functools.partial(kernel, G, F, T, C, J, m, detour),
            out_shape=(
                jax.ShapeDtypeStruct((F * r, cu), bf16),
                jax.ShapeDtypeStruct((m * rd, T * cd), bf16),
                jax.ShapeDtypeStruct((R, D), bf16),
            ),
            in_specs=[pl.BlockSpec(memory_space=pltpu.VMEM)] + [pl.BlockSpec(memory_space=pltpu.HBM)] * 3,
            out_specs=(any_spec,) * 3,
            scratch_shapes=[
                pltpu.VMEM((r, cu), jnp.float32),
                pltpu.VMEM((rd, cd), jnp.float32),
                pltpu.VMEM((R, D), bf16),
                pltpu.VMEM((J, rd, w), bf16),
                pltpu.VMEM((J, rd, w), bf16),
                pltpu.VMEM((T * R, D), bf16),
                pltpu.VMEM((F * r, cu), bf16),
                pltpu.VMEM((T * J, m * rd, w), bf16),
                pltpu.VMEM((T * R, cu), bf16),
                pltpu.VMEM((T * J, T * R, w), bf16),
                pltpu.VMEM((T - 1, T * J, R, w), bf16),
                pltpu.VMEM((R, D), bf16),
                dma((sends,)),
                dma((2, F - 1, C)),
                dma((max(G - 1, 1), 2, F - 1, C)),
                dma((m, T, J)),
                dma((max(G - 1, 1), m, T, J)),
                dma((T,)),
                dma((T - 1, T, J)),
                dma((J,)),
                dma((max(G - 1, 1), J)),
                dma((5 + J + T * J,)),
            ],
            compiler_params=pltpu.CompilerParams(
                collective_id=0, has_side_effects=True, vmem_limit_bytes=VMEM_MIB * 2**20
            ),
        )(norm_gain.reshape(1, r), tokens, up_master, down_master)
        if not FINAL:
            return held
        return pl.pallas_call(
            place,
            out_shape=tuple(jax.ShapeDtypeStruct(a.shape, a.dtype) for a in held),
            in_specs=[any_spec] * 3,
            out_specs=(any_spec,) * 3,
            scratch_shapes=[dma((3,))],
            compiler_params=pltpu.CompilerParams(vmem_limit_bytes=2**20),
        )(*held)

    in_specs = (P(("grp", "fs", "tp"), None), P("fs", "tp"), P("fs", "tp"), P("fs"))
    out_specs = (P("grp", "tp"), P(("grp", "tp"), None), P(("grp", "fs", "tp"), None))
    return jax.shard_map(
        on_device, mesh=mesh, in_specs=in_specs, out_specs=out_specs, check_vma=False
    )
```
